32 devices in a mesh: ep: 8 (over z, x), tp: 4 (over y, core).
Axes of the slice: x: 2, y: 2, z: 4, core: 2. Of those that a mesh axis runs over, the one named last changes fastest.
Arguments:
- tokens: bfloat16 [128, 2048], P('ep'), may hold values from -6 to 6
- lengths: int32 [128], P('ep'), may hold values from 1 to 1024, as said below
- key_cache: bfloat16 [128, 1024, 8, 128], P('ep', None, 'tp'), may hold values from -200 to 200
- value_cache: bfloat16 [128, 1024, 8, 128], P('ep', None, 'tp'), may hold values from -6 to 6
- attn_gain: float32 [2048], replicated, may hold values from 0.1 to 1.9
- w_query: bfloat16 [2048, 8, 128], P(None, 'tp'), may hold values from -0.1875 to 0.1875
- w_key: bfloat16 [2048, 8, 128], P(None, 'tp'), may hold values from -0.15625 to 0.15625
- w_value: bfloat16 [2048, 8, 128], P(None, 'tp'), may hold values from -0.125 to 0.125
- mix_lambda: float32 [8], P('tp'), may hold values from 0.3 to 0.8
- head_gain: float32 [128], replicated, may hold values from 0.1 to 1.9
- w_out: bfloat16 [8, 128, 2048], P('tp'), may hold values from -2.5 to 2.5
- ffn_gain: float32 [2048], replicated, may hold values from 0.1 to 1.9
- w_gate: bfloat16 [8, 2048, 2048], P('ep', None, 'tp'), may hold values from -1 to 1
- w_up: bfloat16 [8, 2048, 2048], P('ep', None, 'tp'), may hold values from -1 to 1
- w_down: bfloat16 [8, 2048, 2048], P('ep', 'tp'), may hold values from -0.046875 to 0.046875
- routes: int32 [128, 4], P('ep'), may hold values from 0 to 7, all different within a row; in each aligned block of 16 rows (0 to 15, 16 to 31, ...) at most 16 rows name the same one
- route_weights: float32 [128, 4], P('ep'), may hold values from 0.1 to 1
Outputs:
- mixed: bfloat16 [128, 2048], P('ep', 'tp')
The draws below stay inside these ranges and needn't reach their ends.
Inputs may be any that keep to these rules, and one draw needn't show every extreme that they name: `routes`: in each aligned block of 16 rows no expert is named by more than 16 entries, and one is named by exactly 16 in some block; each row names 4 different experts. `lengths`: some sequence has all 1024 positions valid.
All inputs are finite; a program needn't handle non-finite values.
Results may differ from the reference program's by a relative error of at most 0.02.
The reference program's roundings to bfloat16 on the way count: a program that leaves them out, or rounds other values in their place, can miss the bound.
Values may be sent and summed in bfloat16 or wider, within the bound.
A program may use at most 128 MiB of HBM per device.

```python
import math
import jax
import jax.numpy as jnp
import numpy as np
from jax import lax

D = 2048
HEADS = 8
HALF = 64
VDIM = 128
FF = 2048
TOP = 4
SEQ_DEV = 16
LEN = 1024
SEQS = 128
EXPERTS = 8
CAP = 16
GROUP_HEADS = 2
FF_DEV = 512
N_TP = 4


def draw_key_cache(key, part):
    base = jnp.clip(jax.random.normal(jax.random.fold_in(key, 11), (SEQS, LEN, HEADS, VDIM), jnp.float32), -6.0, 6.0)
    return base.astype(jnp.bfloat16)


def draw_lengths(key, part):
    groups = SEQS // SEQ_DEV
    limits = jax.random.randint(jax.random.fold_in(key, 21), (groups,), LEN // 8, LEN + 1)
    fullest = jax.random.randint(jax.random.fold_in(key, 22), (), 0, groups)
    group_ids = lax.iota(jnp.int32, groups)
    limits = jnp.where(group_ids == fullest, LEN, limits)
    raw_bits = jax.random.randint(jax.random.fold_in(key, 23), (groups, SEQ_DEV), 0, 1 << 30)
    seq_lengths = raw_bits % limits[:, None] + 1
    chosen_seq = jax.random.randint(jax.random.fold_in(key, 24), (), 0, SEQ_DEV)
    hit = (group_ids[:, None] == fullest) & (lax.iota(jnp.int32, SEQ_DEV)[None, :] == chosen_seq)
    seq_lengths = jnp.where(hit, LEN, seq_lengths)
    return seq_lengths.reshape(SEQS).astype(jnp.int32)


def shard_levels(own_key, shape, cuts, smallest, high):
    factor_of, own = 1.0, jax.random.fold_in(own_key, 6)
    for axis_at, shards_of in cuts:
        draws = jnp.exp(jax.random.uniform(jax.random.fold_in(own, axis_at), (shards_of,), jnp.float32, smallest / len(cuts), high / len(cuts)))
        factor_of = factor_of * jnp.repeat(draws, shape[axis_at] // shards_of).reshape([-1 if axis == axis_at else 1 for axis in range(len(shape))])
    return factor_of


def routed_block(stream_key, own, number, rows, count, top, bound, lean):
    order = jax.random.permutation(stream_key, count)
    heavy_load, usual = portions_of(count, rows * top, bound, lean, True), portions_of(count, rows * top, bound, lean, False)
    places = jnp.arange(count)

    def named(sizes, rotation):
        used = int((sizes > 0).sum())
        fixed = max(1, used // 4)
        moved = fixed + (places - fixed + rotation * (used - fixed)) % max(1, count - fixed)
        return jnp.zeros((count,), jnp.int32).at[order[jnp.where(places < fixed, places, moved)]].set(jnp.asarray(sizes, jnp.int32))

    sizes = jnp.where(number % 4 == 0, named(heavy_load, number // 4), named(usual, number - number // 4 - 1))
    mixed = jax.random.permutation(jax.random.fold_in(own, 3), count)
    source_of, receiver = mixed[0:count // 2 * 2:2], mixed[1:count // 2 * 2:2]
    room = jnp.minimum(sizes[source_of] - 1, bound - sizes[receiver]) // 2
    room = jnp.where((source_of == order[0]) | (receiver == order[0]) | (sizes[receiver] == 0), 0, jnp.maximum(room, 0))
    moved = jax.random.randint(jax.random.fold_in(own, 4), (count // 2,), 0, 1 << 20) % (room + 1)
    sizes = sizes.at[source_of].add(-moved).at[receiver].add(moved)
    members = jnp.searchsorted(jnp.cumsum(sizes), jnp.arange(rows * top), side="right").astype(jnp.int32)
    grid = members.reshape(top, rows).T
    grid = grid[jax.random.permutation(jax.random.fold_in(own, 1), rows)]
    rotation = jax.random.randint(jax.random.fold_in(own, 2), (rows, 1), 0, top)
    return jnp.take_along_axis(grid, (jnp.arange(top)[None, :] + rotation) % top, axis=1)


def portions_of(count, total, bound, slope, full):
    loads = [(1 << 20) // math.isqrt(rank ** slope) + 1 for rank in range(1, count + 1)]
    largest = bound if full else min(bound, max(-(-total // count), total * loads[0] // sum(loads)))
    least = 1 if total - largest >= count - 1 else 0
    holding, spare = [largest] + [least] * (count - 1), total - largest - least * (count - 1)
    while spare > 0:
        free = [i for i in range(1, count) if holding[i] < largest] or [i for i in range(1, count) if holding[i] < bound]
        pool, left = sum([loads[i] for i in free]), spare
        for i in free:
            more = min(bound - holding[i], max(1, left * loads[i] // pool), spare)
            holding[i] = holding[i] + more
            spare = spare - more
    return np.array(holding)


def centred(rng, shape, spread, most, cuts=(), dtype=jnp.bfloat16):
    loudness = shard_levels(rng, shape, cuts, -0.22, 0.18) if cuts else 1.0
    array = jax.random.normal(rng, shape, jnp.float32) * spread * loudness
    return jnp.minimum(jnp.maximum(array, -most), most).astype(dtype)


def setup_inputs(seed: int = 0) -> dict:
    key_of = jax.random.split(jax.random.key(seed), 18)
    tokens = centred(key_of[0], (SEQS, D), 1.0, 6.0, ((0, 8),))
    lengths = draw_lengths(jax.random.fold_in(key_of[17], 71), 0)
    key_cache = draw_key_cache(jax.random.fold_in(key_of[17], 71), 0)
    value_cache = centred(key_of[3], (SEQS, LEN, HEADS, VDIM), 1.0, 6.0, ((0, 8), (2, 4)))
    attn_gain = jnp.clip(1.0 + 0.18 * jax.random.normal(key_of[4], (D,), jnp.float32), 0.1, 1.9)
    w_query = centred(key_of[5], (D, HEADS, VDIM), (D // 2) ** -0.5, 0.1875, ((1, 4),))
    w_key = centred(key_of[6], (D, HEADS, VDIM), (D * 2 // 3) ** -0.5, 0.15625, ((1, 4),))
    w_value = centred(key_of[7], (D, HEADS, VDIM), D ** -0.5, 0.125, ((1, 4),))
    mix_lambda = jnp.clip(0.3 + 0.5 * jax.random.uniform(key_of[8], (HEADS,), jnp.float32) ** shard_levels(key_of[8], (HEADS,), ((0, 4),), -0.2, 0.2), 0.3, 0.8)
    head_gain = jnp.clip(1.0 + 0.18 * jax.random.normal(key_of[9], (VDIM,), jnp.float32), 0.1, 1.9)
    w_out = centred(key_of[10], (HEADS, VDIM, D), (5.0 / (HEADS * VDIM) ** 0.5), 2.5, ((0, 4),))
    ffn_gain = jnp.clip(1.0 + 0.18 * jax.random.normal(key_of[11], (D,), jnp.float32), 0.1, 1.9)
    w_gate = centred(key_of[12], (EXPERTS, D, FF), (3.0 / D ** 0.5), 1.0, ((0, 8), (2, 4)))
    w_up = centred(key_of[13], (EXPERTS, D, FF), (3.0 / D ** 0.5), 1.0, ((0, 8), (2, 4)))
    w_down = centred(key_of[14], (EXPERTS, FF, D), (0.15 / FF ** 0.5), 0.046875, ((0, 8), (1, 4)))
    routes_keys = jax.random.split(jax.random.fold_in(key_of[15], 1), SEQS // SEQ_DEV)
    routes_turns = jax.random.permutation(jax.random.fold_in(key_of[15], 3), SEQS // SEQ_DEV)
    routes = jax.vmap(lambda own, number: routed_block(jax.random.fold_in(key_of[15], 2), own, number, SEQ_DEV, EXPERTS, TOP, CAP, 2))(routes_keys, routes_turns).reshape((SEQS, TOP))
    route_weights = jnp.clip(0.1 + 0.9 * jax.random.uniform(key_of[16], (SEQS, TOP), jnp.float32) ** shard_levels(key_of[16], (SEQS, TOP), ((0, 8),), -0.2, 0.2), 0.1, 1.0)
    return dict(tokens=tokens, lengths=lengths, key_cache=key_cache, value_cache=value_cache, attn_gain=attn_gain, w_query=w_query, w_key=w_key, w_value=w_value, mix_lambda=mix_lambda, head_gain=head_gain, w_out=w_out, ffn_gain=ffn_gain, w_gate=w_gate, w_up=w_up, w_down=w_down, routes=routes, route_weights=route_weights)


epsilon = 1e-06
clamp_limit = 7.0
sigmoid_slope = 1.702
branch_scale = 0.2

def norm_rows(source, gain):
    wide = source.astype(jnp.float32)
    return wide * lax.rsqrt(lax.optimization_barrier(jnp.mean(wide * wide, axis=-1, keepdims=True)) + epsilon) * gain

def reference(tokens, lengths, key_cache, value_cache, attn_gain, w_query, w_key, w_value, mix_lambda, head_gain, w_out, ffn_gain, w_gate, w_up, w_down, routes, route_weights):
    groups = SEQS // SEQ_DEV
    columns = HEADS * VDIM
    normed = norm_rows(tokens, attn_gain).astype(jnp.bfloat16)
    queries = jnp.dot(normed, w_query.reshape(D, columns), preferred_element_type=jnp.float32).astype(jnp.bfloat16)
    key_new = jnp.dot(normed, w_key.reshape(D, columns), preferred_element_type=jnp.float32).astype(jnp.bfloat16)
    value_new = jnp.dot(normed, w_value.reshape(D, columns), preferred_element_type=jnp.float32).astype(jnp.bfloat16)
    halves = (lax.iota(jnp.int32, VDIM) < HALF).astype(jnp.float32)
    selector = jnp.stack([halves, 1.0 - halves])
    score_scale = HALF ** (-0.5)
    positions = lax.iota(jnp.int32, LEN)

    def attend(blocks):
        query_rows, fresh_keys, fresh_values, key_rows, value_rows, seq_lengths = blocks
        query_wide = query_rows.astype(jnp.float32)[:, :, None, :] * selector[None, None]
        scores = jnp.einsum('shcd,slhd->shcl', query_wide, key_rows.astype(jnp.float32)) * score_scale
        own_scores = jnp.einsum('shcd,shd->shc', query_wide, fresh_keys.astype(jnp.float32)) * score_scale
        live_mask = (positions[None, :] < seq_lengths[:, None])[:, None, None, :]
        scores = jnp.where(live_mask, scores, -jnp.inf)
        peak = jnp.maximum(lax.optimization_barrier(jnp.max(scores, axis=-1)), own_scores)
        weights = jnp.exp(scores - peak[..., None])
        own_weight = jnp.exp(own_scores - peak)
        denominator = lax.optimization_barrier(jnp.sum(weights, axis=-1)) + own_weight
        shares = weights / denominator[..., None]
        own_share = own_weight / denominator
        balance = mix_lambda[None, :]
        mix_weights = (shares[:, :, 0] - balance[..., None] * shares[:, :, 1]).astype(jnp.bfloat16)
        own_mixed = (own_share[:, :, 0] - balance * own_share[:, :, 1]).astype(jnp.bfloat16)
        output = jnp.einsum('shl,slhd->shd', mix_weights.astype(jnp.float32), value_rows.astype(jnp.float32))
        return output + own_mixed.astype(jnp.float32)[..., None] * fresh_values.astype(jnp.float32)
    grouped = lax.map(attend, (queries.reshape(groups, SEQ_DEV, HEADS, VDIM), key_new.reshape(groups, SEQ_DEV, HEADS, VDIM), value_new.reshape(groups, SEQ_DEV, HEADS, VDIM), key_cache.reshape(groups, SEQ_DEV, LEN, HEADS, VDIM), value_cache.reshape(groups, SEQ_DEV, LEN, HEADS, VDIM), lengths.reshape(groups, SEQ_DEV)))
    heads_out = grouped.reshape(SEQS, HEADS, VDIM)
    normed_heads = (heads_out * lax.rsqrt(lax.optimization_barrier(jnp.mean(heads_out * heads_out, axis=-1, keepdims=True)) + epsilon) * head_gain * branch_scale).astype(jnp.bfloat16)
    parts = jnp.einsum('sgk,gkd->sgd', normed_heads.reshape(SEQS, N_TP, GROUP_HEADS * VDIM).astype(jnp.float32), w_out.reshape(N_TP, GROUP_HEADS * VDIM, D).astype(jnp.float32))
    attention = lax.optimization_barrier(jnp.sum(lax.optimization_barrier(parts.astype(jnp.bfloat16)).astype(jnp.float32), axis=1))
    residual = (tokens.astype(jnp.float32) + attention).astype(jnp.bfloat16)
    normed_ffn = norm_rows(residual, ffn_gain).astype(jnp.bfloat16)
    entries = routes.reshape(groups, SEQ_DEV * TOP)
    onehot = (entries[..., None] == lax.iota(jnp.int32, EXPERTS)[None, None, :]).astype(jnp.int32)
    entry_slot = lax.optimization_barrier(jnp.sum((jnp.cumsum(onehot, axis=1) - onehot) * onehot, axis=-1))
    target = (entries * CAP + entry_slot).astype(jnp.int32)
    placing = (lax.iota(jnp.int32, EXPERTS * CAP)[None, :, None] == target[:, None, :]).astype(jnp.float32)
    repeated = jnp.repeat(normed_ffn.reshape(groups, SEQ_DEV, D), TOP, axis=1).astype(jnp.float32)
    outgoing = jnp.einsum('gtr,grd->gtd', placing, repeated).astype(jnp.bfloat16)
    by_expert = outgoing.reshape(groups, EXPERTS, CAP, D).transpose(1, 0, 2, 3).reshape(EXPERTS, groups * CAP, D)

    def expert(blocks):
        arrived, gate_weight, up_weight, down_weight = blocks
        gate_value = jnp.minimum(jnp.dot(arrived, gate_weight, preferred_element_type=jnp.float32), clamp_limit)
        up_value = jnp.clip(jnp.dot(arrived, up_weight, preferred_element_type=jnp.float32), -clamp_limit, clamp_limit)
        activated = ((up_value + 1.0) * gate_value * jax.nn.sigmoid(sigmoid_slope * gate_value)).astype(jnp.bfloat16)
        pieces = jnp.einsum('rgf,gfd->rgd', activated.reshape(-1, N_TP, FF_DEV).astype(jnp.float32), down_weight.reshape(N_TP, FF_DEV, D).astype(jnp.float32))
        summed = lax.optimization_barrier(jnp.sum(lax.optimization_barrier(pieces.astype(jnp.bfloat16)).astype(jnp.float32), axis=1))
        return summed.astype(jnp.bfloat16)
    results = lax.map(expert, (by_expert, w_gate, w_up, w_down))
    returned = results.reshape(EXPERTS, groups, CAP, D).transpose(1, 0, 2, 3).reshape(groups, EXPERTS * CAP, D)
    chosen = (lax.iota(jnp.int32, EXPERTS * CAP)[None, None, None, :] == target.reshape(groups, SEQ_DEV, TOP)[..., None]).astype(jnp.float32)
    combine = lax.optimization_barrier(jnp.sum(route_weights.reshape(groups, SEQ_DEV, TOP, 1) * chosen, axis=2))
    expert_sum = jnp.einsum('gsr,grd->gsd', combine, returned.astype(jnp.float32), precision=lax.Precision.HIGHEST)
    return (residual.astype(jnp.float32) + expert_sum.reshape(SEQS, D)).astype(jnp.bfloat16)
```

```python
import functools

import jax
import jax.numpy as jnp
from jax import lax
from jax.experimental import pallas as pl
from jax.experimental.pallas import tpu as pltpu
from jax.sharding import PartitionSpec as P

epsilon = 1e-06
clamp_limit = 7.0
sigmoid_slope = 1.702
branch_scale = 0.2


def norm_rows(source, gain):
    wide = source.astype(jnp.float32)
    return wide * lax.rsqrt(jnp.mean(wide * wide, axis=-1, keepdims=True) + epsilon) * gain


def mixed_weights(scores, own_scores, mix_lambda):
    peak = jnp.maximum(jnp.max(scores, axis=-1), own_scores)
    weights = jnp.exp(scores - peak[..., None])
    own_weight = jnp.exp(own_scores - peak)
    denominator = jnp.sum(weights, axis=-1) + own_weight
    shares = weights / denominator[..., None]
    own_share = own_weight / denominator
    balance = mix_lambda[None, :]
    mix_weights = (shares[:, :, 0] - balance[..., None] * shares[:, :, 1]).astype(jnp.bfloat16)
    own_mixed = (own_share[:, :, 0] - balance * own_share[:, :, 1]).astype(jnp.bfloat16)
    return (mix_weights, own_mixed)


MESH = pl.DeviceIdType.MESH


def exchange_kernel(
    n_ep,
    n_tp,
    heads_ref,
    tokens_ref,
    gain_ref,
    routes_ref,
    route_weights_ref,
    w_out_hbm,
    w_gate_hbm,
    w_up_hbm,
    w_down_hbm,
    out_ref,
    w_out_ref,
    w_gate_ref,
    w_up_ref,
    w_down_ref,
    part_ref,
    part_in_ref,
    rows_ref,
    normed_ref,
    piece_ref,
    piece_in_ref,
    weight_sems,
    part_sems,
    rows_sems,
    piece_sems,
):
    my_ep, my_tp = lax.axis_index("ep"), lax.axis_index("tp")
    n_all = n_ep * n_tp
    me = my_ep * n_tp + my_tp
    seq_dev = tokens_ref.shape[0]
    block = out_ref.shape[1]

    weight_pairs = (
        (w_out_hbm, w_out_ref),
        (w_gate_hbm, w_gate_ref),
        (w_up_hbm, w_up_ref),
        (w_down_hbm, w_down_ref),
    )
    weight_copies = [
        pltpu.make_async_copy(source, target, weight_sems.at[i])
        for i, (source, target) in enumerate(weight_pairs)
    ]
    for copy in weight_copies:
        copy.start()

    barrier = pltpu.get_barrier_semaphore()

    def greet(k, carry):
        peer = lax.rem(me + k, n_all)
        pl.semaphore_signal(
            barrier, inc=1, device_id=(peer // n_tp, lax.rem(peer, n_tp)), device_id_type=MESH
        )
        return carry

    lax.fori_loop(1, n_all, greet, 0)

    weight_copies[0].wait()
    for c in range(n_tp):
        columns = slice(c * block, (c + 1) * block)
        part_ref[c] = jnp.dot(
            heads_ref[...], w_out_ref[:, columns], preferred_element_type=jnp.float32
        ).astype(jnp.bfloat16)
    pl.semaphore_wait(barrier, n_all - 1)

    for k in range(1, n_tp):
        peer = lax.rem(my_tp + k, n_tp)
        pltpu.make_async_remote_copy(
            src_ref=part_ref.at[peer],
            dst_ref=part_in_ref.at[k - 1],
            send_sem=part_sems.at[0],
            recv_sem=part_sems.at[1],
            device_id=(my_ep, peer),
            device_id_type=MESH,
        ).start()
    own_columns = pl.ds(pl.multiple_of(my_tp * block, block), block)
    own_rows = pl.ds(pl.multiple_of(my_ep * seq_dev, seq_dev), seq_dev)
    attention = part_ref[my_tp].astype(jnp.float32)
    if n_tp > 1:
        pltpu.make_async_copy(part_in_ref, part_in_ref, part_sems.at[1]).wait()
        for k in range(1, n_tp):
            attention += part_in_ref[k - 1].astype(jnp.float32)
    residual = (tokens_ref[:, own_columns].astype(jnp.float32) + attention).astype(jnp.bfloat16)
    rows_ref[own_rows, own_columns] = residual

    def spread(k, carry):
        peer = lax.rem(me + k, n_all)
        pltpu.make_async_remote_copy(
            src_ref=rows_ref.at[own_rows, own_columns],
            dst_ref=rows_ref.at[own_rows, own_columns],
            send_sem=rows_sems.at[0],
            recv_sem=rows_sems.at[1],
            device_id=(peer // n_tp, lax.rem(peer, n_tp)),
            device_id_type=MESH,
        ).start()
        return carry

    lax.fori_loop(1, n_all, spread, 0)
    others = piece_in_ref.at[pl.ds(0, n_all - 1)]
    pltpu.make_async_copy(others, others, rows_sems.at[1]).wait()
    pltpu.make_async_copy(others, others, rows_sems.at[0]).wait()
    wide = rows_ref[...].astype(jnp.float32)
    scale = lax.rsqrt(jnp.mean(wide * wide, axis=-1, keepdims=True) + epsilon)
    normed_ref[...] = (wide * scale * gain_ref[...]).astype(jnp.bfloat16)

    weight_copies[1].wait()
    gate_value = jnp.minimum(
        jnp.dot(normed_ref[...], w_gate_ref[...], preferred_element_type=jnp.float32), clamp_limit
    )
    weight_copies[2].wait()
    up_value = jnp.clip(
        jnp.dot(normed_ref[...], w_up_ref[...], preferred_element_type=jnp.float32),
        -clamp_limit,
        clamp_limit,
    )
    activated = ((up_value + 1.0) * gate_value * jax.nn.sigmoid(sigmoid_slope * gate_value)).astype(
        jnp.bfloat16
    )
    weight_copies[3].wait()

    for c in range(n_tp):
        columns = slice(c * block, (c + 1) * block)
        piece = jnp.dot(
            activated, w_down_ref[:, columns], preferred_element_type=jnp.float32
        ).astype(jnp.bfloat16)
        piece_ref[c] = piece.reshape(n_ep, seq_dev, block)

        def hand_out(k, carry):
            peer_ep = lax.rem(my_ep + k, n_ep)

            @pl.when(jnp.logical_or(peer_ep != my_ep, c != my_tp))
            def _():
                pltpu.make_async_remote_copy(
                    src_ref=piece_ref.at[c, peer_ep],
                    dst_ref=piece_in_ref.at[me],
                    send_sem=piece_sems.at[0],
                    recv_sem=piece_sems.at[1],
                    device_id=(peer_ep, c),
                    device_id_type=MESH,
                ).start()

            return carry

        lax.fori_loop(0, n_ep, hand_out, 0)
    piece_in_ref[me] = piece_ref[my_tp, my_ep]
    pltpu.make_async_copy(others, others, piece_sems.at[1]).wait()

    total = rows_ref[own_rows, own_columns].astype(jnp.float32)
    for expert in range(n_ep):
        named = jnp.where(routes_ref[...] == expert, route_weights_ref[...], 0.0)
        weight = jnp.sum(named, axis=1, keepdims=True)
        summed = piece_in_ref[expert * n_tp].astype(jnp.float32)
        for t in range(1, n_tp):
            summed += piece_in_ref[expert * n_tp + t].astype(jnp.float32)
        total += weight * summed.astype(jnp.bfloat16).astype(jnp.float32)
    out_ref[...] = total.astype(jnp.bfloat16)
    pltpu.make_async_copy(others, others, piece_sems.at[0]).wait()
    if n_tp > 1:
        pltpu.make_async_copy(part_in_ref, part_in_ref, part_sems.at[0]).wait()


def exchange_layer(
    heads, tokens, w_out, ffn_gain, routes, route_weights, w_gate, w_up, w_down
):
    n_ep, n_tp = lax.axis_size("ep"), lax.axis_size("tp")
    seq_dev, model_width = tokens.shape
    block = model_width // n_tp
    vmem = pl.BlockSpec(memory_space=pltpu.VMEM)
    anywhere = pl.BlockSpec(memory_space=pl.ANY)
    bf16 = jnp.bfloat16
    return pl.pallas_call(
        functools.partial(exchange_kernel, n_ep, n_tp),
        out_shape=jax.ShapeDtypeStruct((seq_dev, block), bf16),
        in_specs=[vmem] * 5 + [anywhere] * 4,
        out_specs=vmem,
        scratch_shapes=[
            pltpu.VMEM(w_out.shape, bf16),
            pltpu.VMEM(w_gate.shape, bf16),
            pltpu.VMEM(w_up.shape, bf16),
            pltpu.VMEM(w_down.shape, bf16),
            pltpu.VMEM((n_tp, seq_dev, block), bf16),
            pltpu.VMEM((max(n_tp - 1, 1), seq_dev, block), bf16),
            pltpu.VMEM((n_ep * seq_dev, model_width), bf16),
            pltpu.VMEM((n_ep * seq_dev, model_width), bf16),
            pltpu.VMEM((n_tp, n_ep, seq_dev, block), bf16),
            pltpu.VMEM((n_ep * n_tp, seq_dev, block), bf16),
            pltpu.SemaphoreType.DMA((4,)),
            pltpu.SemaphoreType.DMA((2,)),
            pltpu.SemaphoreType.DMA((2,)),
            pltpu.SemaphoreType.DMA((2,)),
        ],
        compiler_params=pltpu.CompilerParams(collective_id=0, has_side_effects=True),
    )(heads, tokens, ffn_gain, routes, route_weights, w_out, w_gate, w_up, w_down)


def per_device(
    tokens,
    lengths,
    key_cache,
    value_cache,
    attn_gain,
    w_query,
    w_key,
    w_value,
    mix_lambda,
    head_gain,
    w_out,
    ffn_gain,
    w_gate,
    w_up,
    w_down,
    routes,
    route_weights,
):
    seq_dev, model_width = tokens.shape
    group_heads = w_query.shape[1]
    head_width = w_query.shape[2]
    half_width = head_width // 2
    columns = group_heads * head_width
    cache_len = key_cache.shape[1]
    normed = norm_rows(tokens, attn_gain).astype(jnp.bfloat16)
    queries = (
        jnp.dot(normed, w_query.reshape(model_width, columns), preferred_element_type=jnp.float32)
        .astype(jnp.bfloat16)
        .reshape(seq_dev, group_heads, head_width)
    )
    key_new = (
        jnp.dot(normed, w_key.reshape(model_width, columns), preferred_element_type=jnp.float32)
        .astype(jnp.bfloat16)
        .reshape(seq_dev, group_heads, head_width)
    )
    value_new = (
        jnp.dot(normed, w_value.reshape(model_width, columns), preferred_element_type=jnp.float32)
        .astype(jnp.bfloat16)
        .reshape(seq_dev, group_heads, head_width)
    )
    halves = (lax.iota(jnp.int32, head_width) < half_width).astype(jnp.bfloat16)
    stacked_query = jnp.stack([queries * halves, queries * (1 - halves)], axis=2)
    score_scale = half_width ** (-0.5)
    own_scores = (
        jnp.einsum("shcd,shd->shc", stacked_query, key_new, preferred_element_type=jnp.float32)
        * score_scale
    )
    positions = lax.iota(jnp.int32, cache_len)
    live_mask = (positions[None, :] < lengths[:, None])[:, None, None, :]
    scores = (
        jnp.einsum("shcd,slhd->shcl", stacked_query, key_cache, preferred_element_type=jnp.float32)
        * score_scale
    )
    scores = jnp.where(live_mask, scores, -jnp.inf)
    mix_weights, own_mixed = mixed_weights(scores, own_scores, mix_lambda)
    heads_out = jnp.einsum(
        "shl,slhd->shd", mix_weights, value_cache, preferred_element_type=jnp.float32
    )
    heads_out = heads_out + own_mixed.astype(jnp.float32)[..., None] * value_new.astype(jnp.float32)
    normed_heads = (
        heads_out
        * lax.rsqrt(jnp.mean(heads_out * heads_out, axis=-1, keepdims=True) + epsilon)
        * head_gain
        * branch_scale
    ).astype(jnp.bfloat16)
    return exchange_layer(
        normed_heads.reshape(seq_dev, columns),
        tokens,
        w_out.reshape(columns, model_width),
        ffn_gain.reshape(1, model_width),
        routes,
        route_weights,
        w_gate[0],
        w_up[0],
        w_down[0],
    )


def solution(mesh):
    placed = (
        P("ep", None),
        P("ep"),
        P("ep", None, "tp", None),
        P("ep", None, "tp", None),
        P(),
        P(None, "tp", None),
        P(None, "tp", None),
        P(None, "tp", None),
        P("tp"),
        P(),
        P("tp", None, None),
        P(),
        P("ep", None, "tp"),
        P("ep", None, "tp"),
        P("ep", "tp", None),
        P("ep", None),
        P("ep", None),
    )
    return jax.shard_map(
        per_device, mesh=mesh, in_specs=placed, out_specs=P("ep", "tp"), check_vma=False
    )
```

```python
import functools

import jax
import jax.numpy as jnp
from jax import lax
from jax.experimental import pallas as pl
from jax.experimental.pallas import tpu as pltpu
from jax.sharding import PartitionSpec as P

epsilon = 1e-06
clamp_limit = 7.0
sigmoid_slope = 1.702
branch_scale = 0.2


def norm_rows(source, gain):
    wide = source.astype(jnp.float32)
    return wide * lax.rsqrt(jnp.mean(wide * wide, axis=-1, keepdims=True) + epsilon) * gain


def mixed_weights(scores, own_scores, mix_lambda):
    peak = jnp.maximum(jnp.max(scores, axis=-1), own_scores)
    weights = jnp.exp(scores - peak[..., None])
    own_weight = jnp.exp(own_scores - peak)
    denominator = jnp.sum(weights, axis=-1) + own_weight
    shares = weights / denominator[..., None]
    own_share = own_weight / denominator
    balance = mix_lambda[None, :]
    mix_weights = (shares[:, :, 0] - balance[..., None] * shares[:, :, 1]).astype(jnp.bfloat16)
    own_mixed = (own_share[:, :, 0] - balance * own_share[:, :, 1]).astype(jnp.bfloat16)
    return (mix_weights, own_mixed)


MESH = pl.DeviceIdType.MESH


def exchange_kernel(
    n_ep,
    n_tp,
    heads_ref,
    tokens_ref,
    gain_ref,
    routes_ref,
    route_weights_ref,
    w_out_hbm,
    w_gate_hbm,
    w_up_hbm,
    w_down_hbm,
    out_ref,
    w_out_ref,
    w_gate_ref,
    w_up_ref,
    w_down_ref,
    part_ref,
    part_in_ref,
    rows_ref,
    normed_ref,
    piece_ref,
    piece_in_ref,
    back_ref,
    back_in_ref,
    weight_sems,
    part_sems,
    rows_sems,
    fan_sems,
    piece_sems,
    back_sems,
):
    my_ep, my_tp = lax.axis_index("ep"), lax.axis_index("tp")
    seq_dev = tokens_ref.shape[0]
    block = out_ref.shape[1]

    weight_pairs = (
        (w_out_hbm, w_out_ref),
        (w_gate_hbm, w_gate_ref),
        (w_up_hbm, w_up_ref),
        (w_down_hbm, w_down_ref),
    )
    weight_copies = [
        pltpu.make_async_copy(source, target, weight_sems.at[i])
        for i, (source, target) in enumerate(weight_pairs)
    ]
    for copy in weight_copies:
        copy.start()

    barrier = pltpu.get_barrier_semaphore()

    for k in range(1, n_ep):
        pl.semaphore_signal(
            barrier, inc=1, device_id=(lax.rem(my_ep + k, n_ep), my_tp), device_id_type=MESH
        )
    for k in range(1, n_tp):
        pl.semaphore_signal(
            barrier, inc=1, device_id=(my_ep, lax.rem(my_tp + k, n_tp)), device_id_type=MESH
        )

    weight_copies[0].wait()
    for c in range(n_tp):
        columns = slice(c * block, (c + 1) * block)
        part_ref[c] = jnp.dot(
            heads_ref[...], w_out_ref[:, columns], preferred_element_type=jnp.float32
        ).astype(jnp.bfloat16)
    pl.semaphore_wait(barrier, n_ep + n_tp - 2)

    for k in range(1, n_tp):
        peer = lax.rem(my_tp + k, n_tp)
        pltpu.make_async_remote_copy(
            src_ref=part_ref.at[peer],
            dst_ref=part_in_ref.at[k - 1],
            send_sem=part_sems.at[0],
            recv_sem=part_sems.at[1],
            device_id=(my_ep, peer),
            device_id_type=MESH,
        ).start()
    own_columns = pl.ds(pl.multiple_of(my_tp * block, block), block)
    own_rows = pl.ds(pl.multiple_of(my_ep * seq_dev, seq_dev), seq_dev)
    attention = part_ref[my_tp].astype(jnp.float32)
    if n_tp > 1:
        pltpu.make_async_copy(part_in_ref, part_in_ref, part_sems.at[1]).wait()
        for k in range(1, n_tp):
            attention += part_in_ref[k - 1].astype(jnp.float32)
    residual = (tokens_ref[:, own_columns].astype(jnp.float32) + attention).astype(jnp.bfloat16)
    rows_ref[own_rows, own_columns] = residual

    far_first = sorted(range(1, n_ep), key=lambda k: -min(k, n_ep - k))

    def rows_copy(source_ep, device, sems, recv):
        place = rows_ref.at[
            pl.ds(pl.multiple_of(source_ep * seq_dev, seq_dev), seq_dev), own_columns
        ]
        return pltpu.make_async_remote_copy(
            src_ref=place,
            dst_ref=place,
            send_sem=sems.at[0],
            recv_sem=sems.at[recv],
            device_id=device,
            device_id_type=MESH,
        )

    for k in far_first:
        rows_copy(my_ep, (lax.rem(my_ep + k, n_ep), my_tp), rows_sems, k).start()
    for k in [0] + far_first[::-1]:
        source_ep = lax.rem(my_ep + n_ep - k, n_ep)
        if k:
            rows_copy(source_ep, (my_ep, my_tp), rows_sems, k).wait_recv()
        for j in range(1, n_tp):
            peer = lax.rem(my_tp + j, n_tp)
            rows_copy(source_ep, (my_ep, peer), fan_sems, 1).start()
    if n_tp > 1:
        pltpu.make_async_copy(piece_in_ref, piece_in_ref, fan_sems.at[1]).wait()
    wide = rows_ref[...].astype(jnp.float32)
    scale = lax.rsqrt(jnp.mean(wide * wide, axis=-1, keepdims=True) + epsilon)
    normed_ref[...] = (wide * scale * gain_ref[...]).astype(jnp.bfloat16)

    weight_copies[1].wait()
    gate_value = jnp.minimum(
        jnp.dot(normed_ref[...], w_gate_ref[...], preferred_element_type=jnp.float32), clamp_limit
    )
    weight_copies[2].wait()
    up_value = jnp.clip(
        jnp.dot(normed_ref[...], w_up_ref[...], preferred_element_type=jnp.float32),
        -clamp_limit,
        clamp_limit,
    )
    activated = ((up_value + 1.0) * gate_value * jax.nn.sigmoid(sigmoid_slope * gate_value)).astype(
        jnp.bfloat16
    )
    weight_copies[3].wait()

    targets = far_first + [0]
    for j in sorted(range(1, n_tp), key=lambda j: -min(j, n_tp - j)) + [0]:
        peer = lax.rem(my_tp + j, n_tp)
        columns = pl.ds(pl.multiple_of(peer * block, block), block)
        piece = jnp.dot(
            activated, w_down_ref[:, columns], preferred_element_type=jnp.float32
        ).astype(jnp.bfloat16)
        piece_ref[j] = piece.reshape(n_ep, seq_dev, block)
        if j:
            for k in targets:
                target_ep = lax.rem(my_ep + k, n_ep)
                pltpu.make_async_remote_copy(
                    src_ref=piece_ref.at[j, target_ep],
                    dst_ref=piece_in_ref.at[target_ep, j - 1],
                    send_sem=fan_sems.at[2],
                    recv_sem=piece_sems.at[k],
                    device_id=(my_ep, peer),
                    device_id_type=MESH,
                ).start()

    for k in targets:
        target_ep = lax.rem(my_ep + k, n_ep)
        summed = piece_ref[0, target_ep].astype(jnp.float32)
        if n_tp > 1:
            landed = piece_in_ref.at[target_ep]
            pltpu.make_async_copy(landed, landed, piece_sems.at[k]).wait()
            for j in range(1, n_tp):
                summed += piece_in_ref[target_ep, j - 1].astype(jnp.float32)
        back_ref[k] = summed.astype(jnp.bfloat16)
        if k:
            pltpu.make_async_remote_copy(
                src_ref=back_ref.at[k],
                dst_ref=back_in_ref.at[k - 1],
                send_sem=back_sems.at[0],
                recv_sem=back_sems.at[k],
                device_id=(target_ep, my_tp),
                device_id_type=MESH,
            ).start()

    total = rows_ref[own_rows, own_columns].astype(jnp.float32)
    eye = lax.broadcasted_iota(jnp.int32, (seq_dev, seq_dev), 0) == lax.broadcasted_iota(
        jnp.int32, (seq_dev, seq_dev), 1
    )
    for k in [0] + far_first[::-1]:
        expert = lax.rem(my_ep + n_ep - k, n_ep)
        named = jnp.where(routes_ref[...] == expert, route_weights_ref[...], 0.0)
        weight = jnp.sum(named, axis=0, keepdims=True)
        weight = jnp.sum(jnp.where(eye, weight, 0.0), axis=1, keepdims=True)
        if k:
            arrived = back_in_ref.at[k - 1]
            pltpu.make_async_copy(arrived, arrived, back_sems.at[k]).wait()
            total += weight * back_in_ref[k - 1].astype(jnp.float32)
        else:
            total += weight * back_ref[0].astype(jnp.float32)
    out_ref[...] = total.astype(jnp.bfloat16)
    if n_ep > 1:
        pltpu.make_async_copy(back_in_ref, back_in_ref, rows_sems.at[0]).wait()
        pltpu.make_async_copy(back_in_ref, back_in_ref, back_sems.at[0]).wait()
    if n_tp > 1:
        pltpu.make_async_copy(part_in_ref, part_in_ref, part_sems.at[0]).wait()
        pltpu.make_async_copy(piece_in_ref, piece_in_ref, fan_sems.at[0]).wait()
        pltpu.make_async_copy(piece_in_ref, piece_in_ref, fan_sems.at[2]).wait()


def exchange_layer(
    heads, tokens, w_out, ffn_gain, routes, route_weights, w_gate, w_up, w_down
):
    n_ep, n_tp = lax.axis_size("ep"), lax.axis_size("tp")
    seq_dev, model_width = tokens.shape
    block = model_width // n_tp
    vmem = pl.BlockSpec(memory_space=pltpu.VMEM)
    anywhere = pl.BlockSpec(memory_space=pl.ANY)
    bf16 = jnp.bfloat16
    return pl.pallas_call(
        functools.partial(exchange_kernel, n_ep, n_tp),
        out_shape=jax.ShapeDtypeStruct((seq_dev, block), bf16),
        in_specs=[vmem] * 5 + [anywhere] * 4,
        out_specs=vmem,
        scratch_shapes=[
            pltpu.VMEM(w_out.shape, bf16),
            pltpu.VMEM(w_gate.shape, bf16),
            pltpu.VMEM(w_up.shape, bf16),
            pltpu.VMEM(w_down.shape, bf16),
            pltpu.VMEM((n_tp, seq_dev, block), bf16),
            pltpu.VMEM((max(n_tp - 1, 1), seq_dev, block), bf16),
            pltpu.VMEM((n_ep * seq_dev, model_width), bf16),
            pltpu.VMEM((n_ep * seq_dev, model_width), bf16),
            pltpu.VMEM((n_tp, n_ep, seq_dev, block), bf16),
            pltpu.VMEM((n_ep, max(n_tp - 1, 1), seq_dev, block), bf16),
            pltpu.VMEM((n_ep, seq_dev, block), bf16),
            pltpu.VMEM((max(n_ep - 1, 1), seq_dev, block), bf16),
            pltpu.SemaphoreType.DMA((4,)),
            pltpu.SemaphoreType.DMA((2,)),
            pltpu.SemaphoreType.DMA((n_ep,)),
            pltpu.SemaphoreType.DMA((3,)),
            pltpu.SemaphoreType.DMA((n_ep,)),
            pltpu.SemaphoreType.DMA((n_ep,)),
        ],
        compiler_params=pltpu.CompilerParams(collective_id=0, has_side_effects=True),
    )(heads, tokens, ffn_gain, routes, route_weights, w_out, w_gate, w_up, w_down)


def per_device(
    tokens,
    lengths,
    key_cache,
    value_cache,
    attn_gain,
    w_query,
    w_key,
    w_value,
    mix_lambda,
    head_gain,
    w_out,
    ffn_gain,
    w_gate,
    w_up,
    w_down,
    routes,
    route_weights,
):
    seq_dev, model_width = tokens.shape
    group_heads = w_query.shape[1]
    head_width = w_query.shape[2]
    half_width = head_width // 2
    columns = group_heads * head_width
    cache_len = key_cache.shape[1]
    normed = norm_rows(tokens, attn_gain).astype(jnp.bfloat16)
    queries = (
        jnp.dot(normed, w_query.reshape(model_width, columns), preferred_element_type=jnp.float32)
        .astype(jnp.bfloat16)
        .reshape(seq_dev, group_heads, head_width)
    )
    key_new = (
        jnp.dot(normed, w_key.reshape(model_width, columns), preferred_element_type=jnp.float32)
        .astype(jnp.bfloat16)
        .reshape(seq_dev, group_heads, head_width)
    )
    value_new = (
        jnp.dot(normed, w_value.reshape(model_width, columns), preferred_element_type=jnp.float32)
        .astype(jnp.bfloat16)
        .reshape(seq_dev, group_heads, head_width)
    )
    halves = (lax.iota(jnp.int32, head_width) < half_width).astype(jnp.bfloat16)
    stacked_query = jnp.stack([queries * halves, queries * (1 - halves)], axis=2)
    score_scale = half_width ** (-0.5)
    own_scores = (
        jnp.einsum("shcd,shd->shc", stacked_query, key_new, preferred_element_type=jnp.float32)
        * score_scale
    )
    positions = lax.iota(jnp.int32, cache_len)
    live_mask = (positions[None, :] < lengths[:, None])[:, None, None, :]
    scores = (
        jnp.einsum("shcd,slhd->shcl", stacked_query, key_cache, preferred_element_type=jnp.float32)
        * score_scale
    )
    scores = jnp.where(live_mask, scores, -jnp.inf)
    mix_weights, own_mixed = mixed_weights(scores, own_scores, mix_lambda)
    heads_out = jnp.einsum(
        "shl,slhd->shd", mix_weights, value_cache, preferred_element_type=jnp.float32
    )
    heads_out = heads_out + own_mixed.astype(jnp.float32)[..., None] * value_new.astype(jnp.float32)
    normed_heads = (
        heads_out
        * lax.rsqrt(jnp.mean(heads_out * heads_out, axis=-1, keepdims=True) + epsilon)
        * head_gain
        * branch_scale
    ).astype(jnp.bfloat16)
    return exchange_layer(
        normed_heads.reshape(seq_dev, columns),
        tokens,
        w_out.reshape(columns, model_width),
        ffn_gain.reshape(1, model_width),
        routes.T,
        route_weights.T,
        w_gate[0],
        w_up[0],
        w_down[0],
    )


def solution(mesh):
    placed = (
        P("ep", None),
        P("ep"),
        P("ep", None, "tp", None),
        P("ep", None, "tp", None),
        P(),
        P(None, "tp", None),
        P(None, "tp", None),
        P(None, "tp", None),
        P("tp"),
        P(),
        P("tp", None, None),
        P(),
        P("ep", None, "tp"),
        P("ep", None, "tp"),
        P("ep", "tp", None),
        P("ep", None),
        P("ep", None),
    )
    return jax.shard_map(
        per_device, mesh=mesh, in_specs=placed, out_specs=P("ep", "tp"), check_vma=False
    )
```
